32 devices in a mesh: sp: 4 (over x, core), dp: 8 (over z, y).
Axes of the slice: x: 2, y: 2, z: 4, core: 2. Of those that a mesh axis runs over, the one named last changes fastest.
Arguments:
- queries: bfloat16 [16, 8, 576, 128], P('dp', None, 'sp'), may hold values from -6 to 6
- keys: bfloat16 [16, 8, 576, 128], P('dp', None, 'sp'), may hold values from -6 to 6
- values: bfloat16 [16, 8, 576, 128], P('dp', None, 'sp'), may hold values from -6 to 6
- in_gate: bfloat16 [16, 8, 576], P('dp', None, 'sp'), may hold values from -5 to 240
- forget_gate: bfloat16 [16, 8, 576], P('dp', None, 'sp'), may hold values from 1 to 20
- out_gate: bfloat16 [16, 8, 576, 128], P('dp', None, 'sp'), may hold values from -6 to 6
- norm_gain: float32 [8, 128], replicated, may hold values from 0.1 to 1.9
- out_weight: bfloat16 [1024, 2048], P(None, 'dp'), may hold values from -0.1875 to 0.1875
Outputs:
- mixed: bfloat16 [16, 576, 2048], P('dp', 'sp')
The draws below stay inside these ranges and needn't reach their ends.
All inputs are finite; a program needn't handle non-finite values.
Results may differ from the reference program's by a relative error of at most 0.0057.
Values may be sent and summed in bfloat16 or wider, within the bound.
A program may use at most 64 MiB of HBM per device.

```python
import jax
import jax.numpy as jnp
from jax import lax

D = 2048
H = 8
DH = 128
BLK = 64
ML_W = 1024
LEN = 576
SEQS = 16


def draw_in_gate(key, part):
    first, second, third = jax.random.split(jax.random.fold_in(key, 11), 3)
    shape = (SEQS, H, LEN)
    result = jnp.clip(jax.random.normal(first, shape, jnp.float32), -5.0, 5.0)
    return result.astype(jnp.bfloat16)


def draw_forget_gate(key, part):
    first, second, third = jax.random.split(jax.random.fold_in(key, 23), 3)
    shape = (SEQS, H, LEN)
    slow_share = 0.5
    slow = jax.random.bernoulli(first, slow_share, (SEQS, H, 1))
    base = jnp.where(slow, jnp.log(0.6 * LEN), jnp.log(60.0))
    noise = jnp.clip(jax.random.normal(second, shape, jnp.float32) * 0.5, -2.0, 2.0)
    block_factor = jax.random.uniform(third, (SEQS, H, LEN // BLK, 1), jnp.float32, -0.7, 0.7)
    block_factor = jnp.broadcast_to(block_factor, (SEQS, H, LEN // BLK, BLK)).reshape(shape)
    return (base + noise + block_factor).astype(jnp.bfloat16)


def shard_levels(own_key, shape, cuts, least, high):
    level = 1.0
    for axis_at, blocks in cuts:
        steps = jax.random.uniform(jax.random.fold_in(jax.random.fold_in(own_key, 6), axis_at), (blocks,), jnp.float32, least / len(cuts), high / len(cuts))
        level = level * jnp.repeat(jnp.exp(steps), shape[axis_at] // blocks).reshape((-1,) + (1,) * (len(shape) - 1 - axis_at))
    return level


def gaussian(own_key, extent, spread, limit, shards=(), held_as=jnp.bfloat16):
    values = spread * jax.random.normal(own_key, extent, jnp.float32)
    if shards:
        values = values * shard_levels(own_key, extent, shards, -0.22, 0.18)
    return jnp.clip(values, -limit, limit).astype(held_as)


def setup_inputs(seed: int = 0) -> dict:
    key_of = jax.random.split(jax.random.key(seed), 9)
    queries = gaussian(key_of[0], (SEQS, H, LEN, DH), 1.0, 6.0, ((0, 8), (2, 4)))
    keys = gaussian(key_of[1], (SEQS, H, LEN, DH), 1.0, 6.0, ((0, 8), (2, 4)))
    values = gaussian(key_of[2], (SEQS, H, LEN, DH), 1.0, 6.0, ((0, 8), (2, 4)))
    in_gate = draw_in_gate(jax.random.fold_in(key_of[8], 71), 0)
    forget_gate = draw_forget_gate(jax.random.fold_in(key_of[8], 71), 0)
    out_gate = gaussian(key_of[5], (SEQS, H, LEN, DH), 1.0, 6.0, ((0, 8), (2, 4)))
    norm_gain = jnp.clip(1.0 + 0.18 * jax.random.normal(key_of[6], (H, DH), jnp.float32), 0.1, 1.9)
    out_weight = gaussian(key_of[7], (ML_W, D), ML_W ** -0.5, 0.1875, ((1, 8),))
    return dict(queries=queries, keys=keys, values=values, in_gate=in_gate, forget_gate=forget_gate, out_gate=out_gate, norm_gain=norm_gain, out_weight=out_weight)


highest = lax.Precision.HIGHEST
norm_eps = 1e-05

def cell_run(query_in, key_in, value_in, input_in, forget_in):
    head_count = query_in.shape[0]
    head_size = query_in.shape[-1]
    blocks = LEN // BLK

    def to_blocks(array):
        shaped = array.astype(jnp.float32).reshape((head_count, blocks, BLK) + array.shape[2:])
        return jnp.swapaxes(shaped, 0, 1)
    query_b = to_blocks(query_in)
    key_b = to_blocks(key_in) * head_size ** (-0.5)
    value_b = to_blocks(value_in)
    input_b = to_blocks(input_in)
    logf_b = jax.nn.log_sigmoid(to_blocks(forget_in))
    causal_mask = jnp.tril(jnp.ones((BLK, BLK), dtype=bool))

    def advance(state_in, inputs):
        memory, normalizer, stabilizer = state_in
        query_c, key_c, value_c, input_c, logf_c = inputs
        cumulative = jnp.cumsum(logf_c, axis=-1)
        log_weights = cumulative[:, :, None] - cumulative[:, None, :] + input_c[:, None, :]
        log_weights = jnp.where(causal_mask, log_weights, -jnp.inf)
        carried_log = cumulative + stabilizer[:, None]
        row_max = jnp.maximum(lax.optimization_barrier(jnp.max(log_weights, axis=-1)), carried_log)
        w_intra = jnp.exp(log_weights - row_max[:, :, None])
        w_inter = jnp.exp(carried_log - row_max)
        scores = jnp.einsum('hld,hsd->hls', query_c, key_c, precision=highest) * w_intra
        numerator = w_inter[:, :, None] * jnp.einsum('hld,hde->hle', query_c, memory, precision=highest)
        numerator = numerator + jnp.einsum('hls,hse->hle', scores, value_c, precision=highest)
        denominator = w_inter * jnp.einsum('hld,hd->hl', query_c, normalizer, precision=highest) + lax.optimization_barrier(jnp.sum(scores, axis=-1))
        cell_out = numerator / jnp.maximum(jnp.abs(denominator), 1.0)[:, :, None]
        block_end = cumulative[:, -1]
        growth = block_end[:, None] - cumulative + input_c
        stab_new = jnp.maximum(block_end + stabilizer, lax.optimization_barrier(jnp.max(growth, axis=-1)))
        w_key = jnp.exp(growth - stab_new[:, None])
        decay_old = jnp.exp(block_end + stabilizer - stab_new)
        memory = decay_old[:, None, None] * memory + jnp.einsum('hs,hsd,hse->hde', w_key, key_c, value_c, precision=highest)
        normalizer = decay_old[:, None] * normalizer + jnp.einsum('hs,hsd->hd', w_key, key_c, precision=highest)
        return ((memory, normalizer, stab_new), cell_out)
    start = (jnp.zeros((head_count, head_size, head_size), jnp.float32), jnp.zeros((head_count, head_size), jnp.float32), jnp.zeros((head_count,), jnp.float32))
    _, cell_out = lax.scan(advance, start, (query_b, key_b, value_b, input_b, logf_b))
    return jnp.swapaxes(cell_out, 0, 1).reshape(head_count, LEN, head_size).astype(jnp.bfloat16)

def reference(queries, keys, values, in_gate, forget_gate, out_gate, norm_gain, out_weight):

    def per_sequence(packed):
        query_s, key_s, value_s, input_s, forget_s, gate_s = packed
        cell_out = cell_run(query_s, key_s, value_s, input_s, forget_s).astype(jnp.float32)
        mean_val = lax.optimization_barrier(jnp.mean(cell_out, axis=-1, keepdims=True))
        centered = cell_out - mean_val
        variance = lax.optimization_barrier(jnp.mean(centered * centered, axis=-1, keepdims=True))
        normed = centered * lax.rsqrt(variance + norm_eps) * norm_gain[:, None, :]
        hidden = (normed * jax.nn.sigmoid(gate_s.astype(jnp.float32))).astype(jnp.bfloat16)
        flat = jnp.swapaxes(hidden, 0, 1).reshape(LEN, -1)
        return jnp.dot(flat, out_weight, preferred_element_type=jnp.float32).astype(jnp.bfloat16)
    return lax.map(per_sequence, (queries, keys, values, in_gate, forget_gate, out_gate))
```

```python
import functools

import jax
import jax.numpy as jnp
from jax import lax
from jax.experimental import pallas as pl
from jax.experimental.pallas import tpu as pltpu
from jax.sharding import PartitionSpec as P

norm_eps = 1e-05
MESH = pl.DeviceIdType.MESH
HIGHEST = lax.Precision.HIGHEST
NEG = -1e30


def nt_dot(a, b, precision=None):
    return lax.dot_general(
        a, b, (((1,), (1,)), ((), ())), precision=precision, preferred_element_type=jnp.float32
    )


def tn_dot(a, b):
    return lax.dot_general(a, b, (((0,), (0,)), ((), ())), preferred_element_type=jnp.float32)


def cell_kernel(
    ranks, heads, group,
    q_ref, k_ref, v_ref, ig_ref, fg_ref, og_ref, gain_ref,
    hid_ref,
    c_in, c_out, a_in, a_out, c_loc, n_loc, gate_row, top_row, end_row,
    c_send, c_recv, a_send, a_recv,
):
    rank = lax.axis_index("sp")
    items, span, head_size = q_ref.shape
    groups = items // group
    key_scale = head_size ** (-0.5)
    right = lax.rem(rank + 1, ranks)
    left = lax.rem(rank + ranks - 1, ranks)

    barrier = pltpu.get_barrier_semaphore()
    for neighbour in (left, right):
        pl.semaphore_signal(barrier, inc=1, device_id={"sp": neighbour}, device_id_type=MESH)

    row_i = lax.broadcasted_iota(jnp.int32, (span, span), 0)
    col_i = lax.broadcasted_iota(jnp.int32, (span, span), 1)
    logf = jax.nn.log_sigmoid(fg_ref[...].astype(jnp.float32))
    cumulative = jnp.dot(
        logf, (row_i <= col_i).astype(jnp.float32), precision=HIGHEST,
        preferred_element_type=jnp.float32,
    )
    gate = ig_ref[...].astype(jnp.float32) - cumulative
    top = jnp.max(gate, axis=1, keepdims=True)
    gate_row[...] = gate
    top_row[...] = jnp.broadcast_to(top, (items, head_size))
    end_row[...] = jnp.broadcast_to(cumulative[:, span - 1 :], (items, head_size))
    w_row = jnp.exp(gate - top) * key_scale
    w_col = nt_dot((row_i == col_i).astype(jnp.float32), w_row, precision=HIGHEST)
    for item in range(items):
        weighted = k_ref[item].astype(jnp.float32) * w_col[:, item : item + 1]
        n_loc[pl.ds(item, 1), :] = jnp.sum(weighted, axis=0, keepdims=True)
        c_loc[item] = tn_dot(weighted.astype(jnp.bfloat16), v_ref[item])

    pl.semaphore_wait(barrier, 2)

    def copies(g):
        part = pl.ds(g * group, group)
        return (
            pltpu.make_async_remote_copy(
                src_ref=c_out.at[part], dst_ref=c_in.at[part],
                send_sem=c_send.at[g], recv_sem=c_recv.at[g],
                device_id={"sp": right}, device_id_type=MESH,
            ),
            pltpu.make_async_remote_copy(
                src_ref=a_out.at[part], dst_ref=a_in.at[part],
                send_sem=a_send.at[g], recv_sem=a_recv.at[g],
                device_id={"sp": right}, device_id_type=MESH,
            ),
        )

    def pass_on(g):
        for j in range(group):
            item = g * group + j
            stab = a_in[item, 1:2, :]
            top_here = top_row[pl.ds(item, 1), :]
            new_top = jnp.maximum(stab, top_here)
            keep = jnp.exp(stab - new_top)
            add = jnp.exp(top_here - new_top)
            c_out[item] = (keep * c_in[item].astype(jnp.float32) + add * c_loc[item]).astype(
                jnp.bfloat16
            )
            a_out[item, 0:1, :] = keep * a_in[item, 0:1, :] + add * n_loc[pl.ds(item, 1), :]
            a_out[item, 1:2, :] = end_row[pl.ds(item, 1), :] + new_top
        for copy in copies(g):
            copy.start()

    @pl.when(rank == 0)
    def _():
        c_in[...] = jnp.zeros_like(c_in)
        a_in[...] = jnp.zeros_like(a_in)

        def first(g, carry):
            pass_on(g)
            return carry

        lax.fori_loop(0, groups, first, 0)

    causal = col_i <= row_i

    def step(g, carry):
        local = []
        for j in range(group):
            item = g * group + j
            masked = jnp.where(causal, gate_row[pl.ds(item, 1), :], NEG)
            top_p = jnp.max(masked, axis=1, keepdims=True)
            scores = nt_dot(q_ref[item], k_ref[item]) * (jnp.exp(masked - top_p) * key_scale)
            inner = jnp.dot(
                scores.astype(jnp.bfloat16), v_ref[item], preferred_element_type=jnp.float32
            )
            local.append((top_p, jnp.sum(scores, axis=1, keepdims=True), inner))

        @pl.when(rank > 0)
        def _():
            for copy in copies(g):
                copy.wait_recv()

        @pl.when(jnp.logical_and(rank > 0, rank < ranks - 1))
        def _():
            pass_on(g)

        for j in range(group):
            item = g * group + j
            top_p, den, inner = local[j]
            stab = a_in[item, 1:2, 0:1]
            both = jnp.maximum(top_p, stab)
            w_intra = jnp.exp(top_p - both)
            w_inter = jnp.exp(stab - both)
            query = q_ref[item]
            num = w_inter * jnp.dot(query, c_in[item], preferred_element_type=jnp.float32)
            num = num + w_intra * inner
            carried = jnp.sum(
                query.astype(jnp.float32) * a_in[item, 0:1, :], axis=1, keepdims=True
            )
            den = w_inter * carried + w_intra * den
            cell = num / jnp.maximum(jnp.abs(den), 1.0)
            cell = cell.astype(jnp.bfloat16).astype(jnp.float32)
            centered = cell - jnp.mean(cell, axis=1, keepdims=True)
            variance = jnp.mean(centered * centered, axis=1, keepdims=True)
            head = lax.rem(item, heads)
            seq = item // heads
            normed = centered * lax.rsqrt(variance + norm_eps) * gain_ref[pl.ds(head, 1), :]
            hidden = normed * jax.nn.sigmoid(og_ref[item].astype(jnp.float32))
            hid_ref[
                pl.ds(pl.multiple_of(seq * span, 16), span),
                pl.ds(pl.multiple_of(head * head_size, head_size), head_size),
            ] = hidden.astype(jnp.bfloat16)
        return carry

    lax.fori_loop(0, groups, step, 0)

    @pl.when(rank < ranks - 1)
    def _():
        def finish(g, carry):
            for copy in copies(g):
                copy.wait_send()
            return carry

        lax.fori_loop(0, groups, finish, 0)


def run_cells(ranks, queries, keys, values, in_gate, forget_gate, out_gate, norm_gain):
    seqs, heads, span, head_size = queries.shape
    items = seqs * heads
    group = 4 if heads % 4 == 0 else 1
    groups = items // group
    vmem = pl.BlockSpec(memory_space=pltpu.VMEM)
    flat = lambda a: a.reshape((items,) + a.shape[2:])
    return pl.pallas_call(
        functools.partial(cell_kernel, ranks, heads, group),
        out_shape=jax.ShapeDtypeStruct((seqs * span, heads * head_size), jnp.bfloat16),
        in_specs=[vmem] * 7,
        out_specs=vmem,
        scratch_shapes=[
            pltpu.VMEM((items, head_size, head_size), jnp.bfloat16),
            pltpu.VMEM((items, head_size, head_size), jnp.bfloat16),
            pltpu.VMEM((items, 8, head_size), jnp.float32),
            pltpu.VMEM((items, 8, head_size), jnp.float32),
            pltpu.VMEM((items, head_size, head_size), jnp.float32),
            pltpu.VMEM((items, head_size), jnp.float32),
            pltpu.VMEM((items, span), jnp.float32),
            pltpu.VMEM((items, head_size), jnp.float32),
            pltpu.VMEM((items, head_size), jnp.float32),
            pltpu.SemaphoreType.DMA((groups,)),
            pltpu.SemaphoreType.DMA((groups,)),
            pltpu.SemaphoreType.DMA((groups,)),
            pltpu.SemaphoreType.DMA((groups,)),
        ],
        compiler_params=pltpu.CompilerParams(collective_id=0, has_side_effects=True),
        cost_estimate=pl.CostEstimate(
            flops=items * span * head_size * 2 * 4 * span, bytes_accessed=40000000, transcendentals=0
        ),
    )(
        flat(queries), flat(keys), flat(values), flat(in_gate), flat(forget_gate),
        flat(out_gate), norm_gain,
    )


def solution(mesh):
    ranks = mesh.shape["sp"]

    def body(queries, keys, values, in_gate, forget_gate, out_gate, norm_gain, out_weight):
        seqs, heads, span, head_size = queries.shape
        hidden = run_cells(
            ranks, queries, keys, values, in_gate, forget_gate, out_gate, norm_gain
        )
        result = jnp.dot(
            hidden,
            lax.all_gather(out_weight, "dp", axis=1, tiled=True),
            preferred_element_type=jnp.float32,
        )
        return result.astype(jnp.bfloat16).reshape(seqs, span, -1)

    return jax.shard_map(
        body,
        mesh=mesh,
        in_specs=(
            P("dp", None, "sp", None),
            P("dp", None, "sp", None),
            P("dp", None, "sp", None),
            P("dp", None, "sp"),
            P("dp", None, "sp"),
            P("dp", None, "sp", None),
            P(),
            P(None, "dp"),
        ),
        out_specs=P("dp", "sp", None),
        check_vma=False,
    )
```

```python
import functools

import jax
import jax.numpy as jnp
from jax import lax
from jax.experimental import pallas as pl
from jax.experimental.pallas import tpu as pltpu
from jax.sharding import PartitionSpec as P

norm_eps = 1e-05
MESH = pl.DeviceIdType.MESH
HIGHEST = lax.Precision.HIGHEST
NEG = -1e30


def nt_dot(a, b, precision=None):
    return lax.dot_general(
        a, b, (((1,), (1,)), ((), ())), precision=precision, preferred_element_type=jnp.float32
    )


def tn_dot(a, b):
    return lax.dot_general(a, b, (((0,), (0,)), ((), ())), preferred_element_type=jnp.float32)


def split_dot(dot, wide, narrow):
    high = wide.astype(jnp.bfloat16)
    low = (wide - high.astype(jnp.float32)).astype(jnp.bfloat16)
    return dot(high, narrow) + dot(low, narrow)


def nn_dot(a, b):
    return jnp.dot(a, b, preferred_element_type=jnp.float32)


class Cell:
    def __init__(self, ranks, heads, group, refs, hid_ref, state, sems):
        self.ranks, self.heads, self.group = ranks, heads, group
        self.q, self.k, self.v, self.ig, self.fg, self.og, self.gain = refs
        self.hid = hid_ref
        (self.c_in, self.c_out, self.a_in, self.a_out, self.c_loc, self.n_loc, self.gate_row,
         self.top_row, self.end_row) = state
        self.sems = sems
        self.rank = lax.axis_index("sp")
        self.items, self.span, self.size = self.q.shape
        self.groups = self.items // group
        self.scale = self.size ** (-0.5)
        self.right = lax.rem(self.rank + 1, ranks)
        self.row_i = lax.broadcasted_iota(jnp.int32, (self.span, self.span), 0)
        self.col_i = lax.broadcasted_iota(jnp.int32, (self.span, self.span), 1)

    def gates(self):
        items, span, size = self.items, self.span, self.size
        logf = jax.nn.log_sigmoid(self.fg[...].astype(jnp.float32))
        cumulative = jnp.dot(
            logf, (self.row_i <= self.col_i).astype(jnp.float32), precision=HIGHEST,
            preferred_element_type=jnp.float32,
        )
        gate = self.ig[...].astype(jnp.float32) - cumulative
        top = jnp.max(gate, axis=1, keepdims=True)
        self.gate_row[...] = gate
        self.top_row[...] = jnp.broadcast_to(top, (items, size))
        self.end_row[...] = jnp.broadcast_to(cumulative[:, span - 1 :], (items, size))
        w_row = jnp.exp(gate - top) * self.scale
        eye = (self.row_i == self.col_i).astype(jnp.float32)
        self.w_col = nt_dot(eye, w_row, precision=HIGHEST)

    def local_states(self):
        for item in range(self.items):
            weighted = self.k[item].astype(jnp.float32) * self.w_col[:, item : item + 1]
            self.n_loc[pl.ds(item, 1), :] = jnp.sum(weighted, axis=0, keepdims=True)
            self.c_loc[item] = split_dot(tn_dot, weighted, self.v[item])

        @pl.when(self.rank == 0)
        def _():
            self.c_in[...] = jnp.zeros_like(self.c_in)
            self.a_in[...] = jnp.zeros_like(self.a_in)

            def first(g, carry):
                self.pass_on(g)
                return carry

            lax.fori_loop(0, self.groups, first, 0)

    def copies(self, g):
        part = pl.ds(g * self.group, self.group)
        c_send, c_recv, a_send, a_recv = self.sems
        return (
            pltpu.make_async_remote_copy(
                src_ref=self.c_out.at[part], dst_ref=self.c_in.at[part],
                send_sem=c_send.at[g], recv_sem=c_recv.at[g],
                device_id={"sp": self.right}, device_id_type=MESH,
            ),
            pltpu.make_async_remote_copy(
                src_ref=self.a_out.at[part], dst_ref=self.a_in.at[part],
                send_sem=a_send.at[g], recv_sem=a_recv.at[g],
                device_id={"sp": self.right}, device_id_type=MESH,
            ),
        )

    def pass_on(self, g):
        for j in range(self.group):
            item = g * self.group + j
            stab = self.a_in[item, 1:2, :]
            top_here = self.top_row[pl.ds(item, 1), :]
            new_top = jnp.maximum(stab, top_here)
            keep = jnp.exp(stab - new_top)
            add = jnp.exp(top_here - new_top)
            self.c_out[item] = (
                keep * self.c_in[item].astype(jnp.float32) + add * self.c_loc[item]
            ).astype(self.c_out.dtype)
            self.a_out[item, 0:1, :] = (
                keep * self.a_in[item, 0:1, :] + add * self.n_loc[pl.ds(item, 1), :]
            )
            self.a_out[item, 1:2, :] = self.end_row[pl.ds(item, 1), :] + new_top
        for copy in self.copies(g):
            copy.start()

    def step(self, g):
        causal = self.col_i <= self.row_i
        local = []
        for j in range(self.group):
            item = g * self.group + j
            masked = jnp.where(causal, self.gate_row[pl.ds(item, 1), :], NEG)
            top_p = jnp.max(masked, axis=1, keepdims=True)
            scores = nt_dot(self.q[item], self.k[item]) * (jnp.exp(masked - top_p) * self.scale)
            inner = split_dot(nn_dot, scores, self.v[item])
            local.append((top_p, jnp.sum(scores, axis=1, keepdims=True), inner))

        @pl.when(self.rank > 0)
        def _():
            for copy in self.copies(g):
                copy.wait_recv()

        @pl.when(jnp.logical_and(self.rank > 0, self.rank < self.ranks - 1))
        def _():
            self.pass_on(g)

        for j in range(self.group):
            item = g * self.group + j
            top_p, den, inner = local[j]
            stab = self.a_in[item, 1:2, 0:1]
            both = jnp.maximum(top_p, stab)
            w_intra = jnp.exp(top_p - both)
            w_inter = jnp.exp(stab - both)
            query = self.q[item]
            num = w_inter * nn_dot(query, self.c_in[item]) + w_intra * inner
            carried = jnp.sum(
                query.astype(jnp.float32) * self.a_in[item, 0:1, :], axis=1, keepdims=True
            )
            den = w_inter * carried + w_intra * den
            cell = num / jnp.maximum(jnp.abs(den), 1.0)
            cell = cell.astype(jnp.bfloat16).astype(jnp.float32)
            centered = cell - jnp.mean(cell, axis=1, keepdims=True)
            variance = jnp.mean(centered * centered, axis=1, keepdims=True)
            head = lax.rem(item, self.heads)
            seq = item // self.heads
            normed = centered * lax.rsqrt(variance + norm_eps) * self.gain[pl.ds(head, 1), :]
            hidden = normed * jax.nn.sigmoid(self.og[item].astype(jnp.float32))
            self.hid[
                pl.ds(pl.multiple_of(seq * self.span, 16), self.span),
                pl.ds(pl.multiple_of(head * self.size, self.size), self.size),
            ] = hidden.astype(jnp.bfloat16)

    def steps(self, begin, end):
        def one(g, carry):
            self.step(g)
            return carry

        lax.fori_loop(begin, end, one, 0)

    def finish(self):
        @pl.when(self.rank < self.ranks - 1)
        def _():
            def one(g, carry):
                for copy in self.copies(g):
                    copy.wait_send()
                return carry

            lax.fori_loop(0, self.groups, one, 0)


def state_scratch(items, span, size):
    return [
        pltpu.VMEM((items, size, size), jnp.bfloat16),
        pltpu.VMEM((items, size, size), jnp.bfloat16),
        pltpu.VMEM((items, 8, size), jnp.float32),
        pltpu.VMEM((items, 8, size), jnp.float32),
        pltpu.VMEM((items, size, size), jnp.float32),
        pltpu.VMEM((items, size), jnp.float32),
        pltpu.VMEM((items, span), jnp.float32),
        pltpu.VMEM((items, size), jnp.float32),
        pltpu.VMEM((items, size), jnp.float32),
    ]


def cell_kernel(ranks, heads, group, *refs):
    inputs, hid_ref, state, sems = refs[:7], refs[7], refs[8:17], refs[17:21]
    rank = lax.axis_index("sp")
    barrier = pltpu.get_barrier_semaphore()
    for neighbour in (lax.rem(rank + 1, ranks), lax.rem(rank + ranks - 1, ranks)):
        pl.semaphore_signal(barrier, inc=1, device_id={"sp": neighbour}, device_id_type=MESH)
    cell = Cell(ranks, heads, group, inputs, hid_ref, state, sems)
    cell.gates()
    pl.semaphore_wait(barrier, 2)
    cell.local_states()
    cell.steps(0, cell.groups)
    cell.finish()


def nearest(z, nz, k):
    near = jnp.minimum(z, nz - 1 - z)
    half = (k + 1) // 2
    inside = jnp.where(k % 2 == 1, z - half, z + half)
    outside = jnp.where(2 * z < nz, k, nz - 1 - k)
    return jnp.where(k <= 2 * near, inside, outside)


class Gather:
    def __init__(self, nz, ny, w_buf, sems):
        self.nz, self.ny, self.w = nz, ny, w_buf
        (self.z_send, self.z_recv, self.y_send, self.y_recv, self.x_send, self.x_recv,
         self.d_send, self.d_recv) = sems
        self.rank = lax.axis_index("sp")
        self.dp = lax.axis_index("dp")
        self.z, self.y = self.dp // ny, lax.rem(self.dp, ny)
        self.core = lax.rem(self.rank, 2)
        self.plane = lax.rem(self.rank // 2, 2)
        self.sibling = self.rank + 1 - 2 * self.core
        self.across = self.rank + 2 - 4 * self.plane
        self.peer_y = 1 - self.y
        self.rows = w_buf.shape[1] // 2
        self.own = self.dp

    def place(self, k):
        return nearest(self.z, self.nz, k)

    def area(self, piece, part):
        quarter = self.rows // 4
        base = self.core * self.rows
        if part == 1:
            return self.w.at[piece, pl.ds(pl.multiple_of(base + quarter, quarter), 2 * quarter)]
        shift = 3 * self.plane if part == 0 else 3 * (1 - self.plane)
        return self.w.at[piece, pl.ds(pl.multiple_of(base + shift * quarter, quarter), quarter)]

    def copy(self, piece, part, send, recv, where):
        area = self.area(piece, part)
        return pltpu.make_async_remote_copy(
            src_ref=area, dst_ref=area, send_sem=send, recv_sem=recv,
            device_id=where, device_id_type=MESH,
        )

    def z_copy(self, place, part, way):
        ahead = self.z + 1 - 2 * way
        return self.copy(
            place * self.ny + self.y, part, self.z_send.at[place, part, way],
            self.z_recv.at[place, part], {"dp": ahead * self.ny + self.y},
        )

    def y_copy(self, place, mine, part):
        side = self.y if mine else self.peer_y
        return self.copy(
            place * self.ny + side, part, self.y_send.at[place, part],
            self.y_recv.at[place, part], {"dp": self.z * self.ny + self.peer_y},
        )

    def x_copy(self, piece, part):
        return self.copy(
            piece, part, self.x_send.at[piece], self.x_recv.at[piece], {"sp": self.across}
        )

    def d_copy(self, piece, part):
        return self.copy(
            piece, part, self.d_send.at[piece, part], self.d_recv.at[piece, part],
            {"sp": self.sibling},
        )

    def greet(self, barrier, ranks):
        sp = (lax.rem(self.rank + 1, ranks), lax.rem(self.rank + ranks - 1, ranks),
              self.sibling, self.across)
        for one in sp:
            pl.semaphore_signal(barrier, inc=1, device_id={"sp": one}, device_id_type=MESH)
        up, down = lax.rem(self.z + 1, self.nz), lax.rem(self.z + self.nz - 1, self.nz)
        for z, y in ((up, self.y), (down, self.y), (self.z, self.peer_y)):
            pl.semaphore_signal(
                barrier, inc=1, device_id={"dp": z * self.ny + y}, device_id_type=MESH
            )
        return 7

    def start(self):
        for part in (0, 1):
            for way in (0, 1):
                @pl.when(self.z < self.nz - 1 if way == 0 else self.z > 0)
                def _():
                    self.z_copy(self.z, part, way).start()

            self.y_copy(self.z, True, part).start()

    def on_z(self, k):
        place = self.place(k)
        piece = place * self.ny + self.y
        for part in (0, 1):
            self.z_copy(place, part, 0).wait_recv()

            @pl.when(jnp.logical_and(place < self.z, self.z < self.nz - 1))
            def _():
                self.z_copy(place, part, 0).start()

            @pl.when(jnp.logical_and(place > self.z, self.z > 0))
            def _():
                self.z_copy(place, part, 1).start()

            self.y_copy(place, True, part).start()
            if part == 0:
                self.x_copy(piece, 0).start()
            self.d_copy(piece, part).start()

    def on_y(self, k):
        place = self.place(k)
        piece = place * self.ny + self.peer_y
        for part in (0, 1):
            self.y_copy(place, False, part).wait_recv()
            if part == 0:
                self.x_copy(piece, 0).start()
            self.d_copy(piece, part).start()

    def piece_at(self, k, mine):
        return self.place(k) * self.ny + (self.y if mine else self.peer_y)

    def on_x(self, k, mine):
        piece = self.piece_at(k, mine)
        self.x_copy(piece, 2).wait_recv()
        self.d_copy(piece, 2).start()

    def landed(self, k, mine):
        piece = self.piece_at(k, mine)
        other = Gather.__new__(Gather)
        other.__dict__.update(self.__dict__)
        other.core = 1 - self.core
        for part in (0, 1, 2):
            other.d_copy(piece, part).wait_recv()

    def finish(self):
        def z_all(k, carry):
            place = self.place(k)
            for part in (0, 1):
                @pl.when(jnp.logical_and(place <= self.z, self.z < self.nz - 1))
                def _():
                    self.z_copy(place, part, 0).wait_send()

                @pl.when(jnp.logical_and(place >= self.z, self.z > 0))
                def _():
                    self.z_copy(place, part, 1).wait_send()

                self.y_copy(place, True, part).wait_send()
            return carry

        lax.fori_loop(0, self.nz, z_all, 0)

        def others(i, carry):
            piece = lax.rem(self.dp + i, self.nz * self.ny)
            self.x_copy(piece, 0).wait_send()
            for part in (0, 1, 2):
                self.d_copy(piece, part).wait_send()
            return carry

        lax.fori_loop(1, self.nz * self.ny, others, 0)


def whole_kernel(ranks, heads, group, nz, ny, *refs):
    (q_hbm, k_hbm, v_hbm, ig_ref, fg_ref, og_hbm, gain_ref, w_hbm), refs = refs[:8], refs[8:]
    out_hbm, refs = refs[0], refs[1:]
    (q_ref, k_ref, v_ref, og_ref, w_buf, hid_ref, out_ref), refs = refs[:7], refs[7:]
    state, refs = refs[:9], refs[9:]
    chain_sems, refs = refs[:4], refs[4:]
    gather_sems, (load_sems, out_sems) = refs[:8], refs[8:]
    gather = Gather(nz, ny, w_buf, gather_sems)
    barrier = pltpu.get_barrier_semaphore()
    greeted = gather.greet(barrier, ranks)
    w_load = pltpu.make_async_copy(w_hbm, w_buf.at[gather.own], load_sems.at[0])
    loads = [
        pltpu.make_async_copy(src, dst, load_sems.at[1 + i])
        for i, (src, dst) in enumerate(
            ((k_hbm, k_ref), (v_hbm, v_ref), (q_hbm, q_ref), (og_hbm, og_ref))
        )
    ]
    w_load.start()
    for load in loads:
        load.start()
    cell = Cell(
        ranks, heads, group, (q_ref, k_ref, v_ref, ig_ref, fg_ref, og_ref, gain_ref), hid_ref,
        state, chain_sems,
    )
    w_load.wait()
    pl.semaphore_wait(barrier, greeted)
    gather.start()
    cell.gates()
    for load in loads:
        load.wait()
    cell.local_states()
    half = cell.groups // 2

    def out_copy(piece):
        columns = w_buf.shape[2]
        part = pl.ds(pl.multiple_of(piece * columns, columns), columns)
        return pltpu.make_async_copy(
            out_ref.at[:, part], out_hbm.at[:, part], out_sems.at[piece]
        )

    def project(piece):
        columns = w_buf.shape[2]
        part = pl.ds(pl.multiple_of(piece * columns, columns), columns)
        out_ref[:, part] = nn_dot(hid_ref[...], w_buf[piece]).astype(jnp.bfloat16)
        out_copy(piece).start()

    gather.on_z(1)
    gather.on_y(0)
    cell.steps(0, half)
    for k in range(2, nz):
        gather.on_z(k)
        gather.on_y(k - 1)
        gather.on_x(k - 1, True)
        gather.on_x(k - 2, False)
        if k == 2:
            cell.steps(half, cell.groups)
    gather.on_y(nz - 1)
    gather.on_x(nz - 1, True)
    gather.on_x(nz - 2, False)
    project(gather.own)

    def rest(k, carry):
        gather.landed(k, True)
        project(gather.piece_at(k, True))
        gather.landed(k - 1, False)
        project(gather.piece_at(k - 1, False))
        return carry

    lax.fori_loop(1, nz, rest, 0)
    gather.on_x(nz - 1, False)
    gather.landed(nz - 1, False)
    project(gather.piece_at(nz - 1, False))
    cell.finish()
    gather.finish()

    def drain(piece, carry):
        out_copy(piece).wait()
        return carry

    lax.fori_loop(0, nz * ny, drain, 0)


def run_whole(ranks, dps, queries, keys, values, in_gate, forget_gate, out_gate, norm_gain, weight):
    seqs, heads, span, size = queries.shape
    items = seqs * heads
    group = 4
    groups = items // group
    ny = 2
    nz = dps // ny
    rows, columns = weight.shape
    vmem = pl.BlockSpec(memory_space=pltpu.VMEM)
    hbm = pl.BlockSpec(memory_space=pl.ANY)
    flat = lambda a: a.reshape((items,) + a.shape[2:])
    dma = pltpu.SemaphoreType.DMA
    big = pltpu.VMEM((items, span, size), jnp.bfloat16)
    return pl.pallas_call(
        functools.partial(whole_kernel, ranks, heads, group, nz, ny),
        out_shape=jax.ShapeDtypeStruct((seqs * span, dps * columns), jnp.bfloat16),
        in_specs=[hbm, hbm, hbm, vmem, vmem, hbm, vmem, hbm],
        out_specs=hbm,
        scratch_shapes=[
            big, big, big, big,
            pltpu.VMEM((dps, rows, columns), jnp.bfloat16),
            pltpu.VMEM((seqs * span, heads * size), jnp.bfloat16),
            pltpu.VMEM((seqs * span, dps * columns), jnp.bfloat16),
            *state_scratch(items, span, size),
            dma((groups,)), dma((groups,)), dma((groups,)), dma((groups,)),
            dma((nz, 2, 2)), dma((nz, 2)), dma((nz, 2)), dma((nz, 2)),
            dma((dps,)), dma((dps,)), dma((dps, 3)), dma((dps, 3)),
            dma((5,)), dma((dps,)),
        ],
        compiler_params=pltpu.CompilerParams(collective_id=0, has_side_effects=True),
    )(
        flat(queries), flat(keys), flat(values), flat(in_gate), flat(forget_gate),
        flat(out_gate), norm_gain, weight,
    )


def run_cells(ranks, queries, keys, values, in_gate, forget_gate, out_gate, norm_gain):
    seqs, heads, span, head_size = queries.shape
    items = seqs * heads
    group = 4 if heads % 4 == 0 else 1
    groups = items // group
    vmem = pl.BlockSpec(memory_space=pltpu.VMEM)
    flat = lambda a: a.reshape((items,) + a.shape[2:])
    return pl.pallas_call(
        functools.partial(cell_kernel, ranks, heads, group),
        out_shape=jax.ShapeDtypeStruct((seqs * span, heads * head_size), jnp.bfloat16),
        in_specs=[vmem] * 7,
        out_specs=vmem,
        scratch_shapes=[
            *state_scratch(items, span, head_size),
            pltpu.SemaphoreType.DMA((groups,)),
            pltpu.SemaphoreType.DMA((groups,)),
            pltpu.SemaphoreType.DMA((groups,)),
            pltpu.SemaphoreType.DMA((groups,)),
        ],
        compiler_params=pltpu.CompilerParams(collective_id=0, has_side_effects=True),
        cost_estimate=pl.CostEstimate(
            flops=items * span * head_size * 2 * 4 * span, bytes_accessed=40000000, transcendentals=0
        ),
    )(
        flat(queries), flat(keys), flat(values), flat(in_gate), flat(forget_gate),
        flat(out_gate), norm_gain,
    )


def solution(mesh):
    ranks, dps = mesh.shape["sp"], mesh.shape["dp"]

    def body(queries, keys, values, in_gate, forget_gate, out_gate, norm_gain, out_weight):
        seqs, heads, span, head_size = queries.shape
        rows, columns = out_weight.shape
        fits = columns % 128 == 0 and rows % 128 == 0 and dps * rows * columns <= 4 * 2**20
        if ranks == 4 and dps % 2 == 0 and dps >= 6 and heads % 4 == 0 and fits:
            result = run_whole(
                ranks, dps, queries, keys, values, in_gate, forget_gate, out_gate, norm_gain,
                out_weight,
            )
            return result.reshape(seqs, span, -1)
        hidden = run_cells(
            ranks, queries, keys, values, in_gate, forget_gate, out_gate, norm_gain
        )
        result = jnp.dot(
            hidden,
            lax.all_gather(out_weight, "dp", axis=1, tiled=True),
            preferred_element_type=jnp.float32,
        )
        return result.astype(jnp.bfloat16).reshape(seqs, span, -1)

    return jax.shard_map(
        body,
        mesh=mesh,
        in_specs=(
            P("dp", None, "sp", None),
            P("dp", None, "sp", None),
            P("dp", None, "sp", None),
            P("dp", None, "sp"),
            P("dp", None, "sp"),
            P("dp", None, "sp", None),
            P(),
            P(None, "dp"),
        ),
        out_specs=P("dp", "sp", None),
        check_vma=False,
    )
```

```python
import functools

import jax
import jax.numpy as jnp
from jax import lax
from jax.experimental import pallas as pl
from jax.experimental.pallas import tpu as pltpu
from jax.sharding import PartitionSpec as P

norm_eps = 1e-05
MESH = pl.DeviceIdType.MESH
HIGHEST = lax.Precision.HIGHEST
NEG = -1e30


def nt_dot(a, b, precision=None):
    return lax.dot_general(
        a, b, (((1,), (1,)), ((), ())), precision=precision, preferred_element_type=jnp.float32
    )


def tn_dot(a, b):
    return lax.dot_general(a, b, (((0,), (0,)), ((), ())), preferred_element_type=jnp.float32)


def split_dot(dot, wide, narrow):
    high = wide.astype(jnp.bfloat16)
    low = (wide - high.astype(jnp.float32)).astype(jnp.bfloat16)
    return dot(high, narrow) + dot(low, narrow)


def nn_dot(a, b):
    return jnp.dot(a, b, preferred_element_type=jnp.float32)


class Cell:
    def __init__(self, ranks, heads, group, refs, hid_ref, state, sems):
        self.ranks, self.heads, self.group = ranks, heads, group
        self.q, self.k, self.v, self.ig, self.fg, self.og, self.gain = refs
        self.hid = hid_ref
        (self.c_in, self.c_out, self.a_in, self.a_out, self.c_loc, self.n_loc, self.gate_row,
         self.top_row, self.end_row, self.inner, self.stat) = state
        self.sems = sems
        self.rank = lax.axis_index("sp")
        self.items, self.span, self.size = self.q.shape
        self.groups = self.items // group
        self.scale = self.size ** (-0.5)
        self.right = lax.rem(self.rank + 1, ranks)
        self.row_i = lax.broadcasted_iota(jnp.int32, (self.span, self.span), 0)
        self.col_i = lax.broadcasted_iota(jnp.int32, (self.span, self.span), 1)

    def gates(self):
        items, span, size = self.items, self.span, self.size
        logf = jax.nn.log_sigmoid(self.fg[...].astype(jnp.float32))
        cumulative = jnp.dot(
            logf, (self.row_i <= self.col_i).astype(jnp.float32), precision=HIGHEST,
            preferred_element_type=jnp.float32,
        )
        gate = self.ig[...].astype(jnp.float32) - cumulative
        top = jnp.max(gate, axis=1, keepdims=True)
        self.gate_row[...] = gate
        self.top_row[...] = jnp.broadcast_to(top, (items, size))
        self.end_row[...] = jnp.broadcast_to(cumulative[:, span - 1 :], (items, size))
        w_row = jnp.exp(gate - top) * self.scale
        eye = (self.row_i == self.col_i).astype(jnp.float32)
        self.w_col = nt_dot(eye, w_row, precision=HIGHEST)

    def local_states(self):
        for item in range(self.items):
            weighted = self.k[item].astype(jnp.float32) * self.w_col[:, item : item + 1]
            self.n_loc[pl.ds(item, 1), :] = jnp.sum(weighted, axis=0, keepdims=True)
            self.c_loc[item] = split_dot(tn_dot, weighted, self.v[item])

        @pl.when(self.rank == 0)
        def _():
            self.c_in[...] = jnp.zeros_like(self.c_in)
            self.a_in[...] = jnp.zeros_like(self.a_in)

            def first(g, carry):
                self.pass_on(g)
                return carry

            lax.fori_loop(0, self.groups, first, 0)

    def copies(self, g):
        part = pl.ds(g * self.group, self.group)
        c_send, c_recv, a_send, a_recv = self.sems
        return (
            pltpu.make_async_remote_copy(
                src_ref=self.c_out.at[part], dst_ref=self.c_in.at[part],
                send_sem=c_send.at[g], recv_sem=c_recv.at[g],
                device_id={"sp": self.right}, device_id_type=MESH,
            ),
            pltpu.make_async_remote_copy(
                src_ref=self.a_out.at[part], dst_ref=self.a_in.at[part],
                send_sem=a_send.at[g], recv_sem=a_recv.at[g],
                device_id={"sp": self.right}, device_id_type=MESH,
            ),
        )

    def pass_on(self, g):
        for j in range(self.group):
            item = g * self.group + j
            stab = self.a_in[item, 1:2, :]
            top_here = self.top_row[pl.ds(item, 1), :]
            new_top = jnp.maximum(stab, top_here)
            keep = jnp.exp(stab - new_top)
            add = jnp.exp(top_here - new_top)
            self.c_out[item] = (
                keep * self.c_in[item].astype(jnp.float32) + add * self.c_loc[item]
            ).astype(self.c_out.dtype)
            self.a_out[item, 0:1, :] = (
                keep * self.a_in[item, 0:1, :] + add * self.n_loc[pl.ds(item, 1), :]
            )
            self.a_out[item, 1:2, :] = self.end_row[pl.ds(item, 1), :] + new_top
        for copy in self.copies(g):
            copy.start()

    def intra(self, g):
        causal = self.col_i <= self.row_i
        for j in range(self.group):
            item = g * self.group + j
            masked = jnp.where(causal, self.gate_row[pl.ds(item, 1), :], NEG)
            top_p = jnp.max(masked, axis=1, keepdims=True)
            scores = nt_dot(self.q[item], self.k[item]) * (jnp.exp(masked - top_p) * self.scale)
            self.inner[item] = split_dot(nn_dot, scores, self.v[item])
            self.stat[item, :, 0:1] = top_p
            self.stat[item, :, 1:2] = jnp.sum(scores, axis=1, keepdims=True)

    def arrive(self, g):
        for copy in self.copies(g):
            copy.wait_recv()

    def relay(self, g):
        self.arrive(g)
        self.pass_on(g)

    def outcome(self, g):
        for j in range(self.group):
            item = g * self.group + j
            top_p, den = self.stat[item, :, 0:1], self.stat[item, :, 1:2]
            stab = self.a_in[item, 1:2, 0:1]
            both = jnp.maximum(top_p, stab)
            w_intra = jnp.exp(top_p - both)
            w_inter = jnp.exp(stab - both)
            query = self.q[item]
            num = w_inter * nn_dot(query, self.c_in[item]) + w_intra * self.inner[item]
            carried = jnp.sum(
                query.astype(jnp.float32) * self.a_in[item, 0:1, :], axis=1, keepdims=True
            )
            den = w_inter * carried + w_intra * den
            cell = num / jnp.maximum(jnp.abs(den), 1.0)
            cell = cell.astype(jnp.bfloat16).astype(jnp.float32)
            centered = cell - jnp.mean(cell, axis=1, keepdims=True)
            variance = jnp.mean(centered * centered, axis=1, keepdims=True)
            head = lax.rem(item, self.heads)
            seq = item // self.heads
            normed = centered * lax.rsqrt(variance + norm_eps) * self.gain[pl.ds(head, 1), :]
            hidden = normed * jax.nn.sigmoid(self.og[item].astype(jnp.float32))
            self.hid[
                pl.ds(pl.multiple_of(seq * self.span, 16), self.span),
                pl.ds(pl.multiple_of(head * self.size, self.size), self.size),
            ] = hidden.astype(jnp.bfloat16)

    def over(self, work, begin, end):
        def one(g, carry):
            work(g)
            return carry

        lax.fori_loop(begin, end, one, 0)

    def relays(self, ranks, begin, end):
        for rank in ranks:
            @pl.when(self.rank == rank)
            def _():
                self.over(self.relay if rank < self.ranks - 1 else self.arrive, begin, end)

    def finish(self):
        @pl.when(self.rank < self.ranks - 1)
        def _():
            def one(g, carry):
                for copy in self.copies(g):
                    copy.wait_send()
                return carry

            lax.fori_loop(0, self.groups, one, 0)


def state_scratch(items, span, size):
    return [
        pltpu.VMEM((items, size, size), jnp.bfloat16),
        pltpu.VMEM((items, size, size), jnp.bfloat16),
        pltpu.VMEM((items, 8, size), jnp.float32),
        pltpu.VMEM((items, 8, size), jnp.float32),
        pltpu.VMEM((items, size, size), jnp.float32),
        pltpu.VMEM((items, size), jnp.float32),
        pltpu.VMEM((items, span), jnp.float32),
        pltpu.VMEM((items, size), jnp.float32),
        pltpu.VMEM((items, size), jnp.float32),
        pltpu.VMEM((items, span, size), jnp.float32),
        pltpu.VMEM((items, span, size), jnp.float32),
    ]


def cell_kernel(ranks, heads, group, *refs):
    inputs, hid_ref, state, sems = refs[:7], refs[7], refs[8:19], refs[19:23]
    rank = lax.axis_index("sp")
    barrier = pltpu.get_barrier_semaphore()
    for neighbour in (lax.rem(rank + 1, ranks), lax.rem(rank + ranks - 1, ranks)):
        pl.semaphore_signal(barrier, inc=1, device_id={"sp": neighbour}, device_id_type=MESH)
    cell = Cell(ranks, heads, group, inputs, hid_ref, state, sems)
    cell.gates()
    pl.semaphore_wait(barrier, 2)
    cell.local_states()
    cell.over(cell.intra, 0, cell.groups)
    cell.relays(range(1, ranks), 0, cell.groups)
    cell.over(cell.outcome, 0, cell.groups)
    cell.finish()


def nearest(z, nz, k):
    near = jnp.minimum(z, nz - 1 - z)
    half = (k + 1) // 2
    inside = jnp.where(k % 2 == 1, z - half, z + half)
    outside = jnp.where(2 * z < nz, k, nz - 1 - k)
    return jnp.where(k <= 2 * near, inside, outside)


class Gather:
    def __init__(self, nz, ny, w_buf, sems):
        self.nz, self.ny, self.w = nz, ny, w_buf
        (self.z_send, self.z_recv, self.y_send, self.y_recv, self.x_send, self.x_recv,
         self.d_send, self.d_recv) = sems
        self.rank = lax.axis_index("sp")
        self.dp = lax.axis_index("dp")
        self.z, self.y = self.dp // ny, lax.rem(self.dp, ny)
        self.core = lax.rem(self.rank, 2)
        self.plane = lax.rem(self.rank // 2, 2)
        self.sibling = self.rank + 1 - 2 * self.core
        self.across = self.rank + 2 - 4 * self.plane
        self.peer_y = 1 - self.y
        self.rows = w_buf.shape[1] // 2
        self.own = self.dp

    def place(self, k):
        return nearest(self.z, self.nz, k)

    def area(self, piece, part):
        quarter = self.rows // 4
        base = self.core * self.rows
        shift = (3 * self.plane, 1, 2, 3 * (1 - self.plane))[part]
        return self.w.at[piece, pl.ds(pl.multiple_of(base + shift * quarter, quarter), quarter)]

    def copy(self, piece, part, send, recv, where):
        area = self.area(piece, part)
        return pltpu.make_async_remote_copy(
            src_ref=area, dst_ref=area, send_sem=send, recv_sem=recv,
            device_id=where, device_id_type=MESH,
        )

    def z_copy(self, place, part, way):
        ahead = self.z + 1 - 2 * way
        return self.copy(
            place * self.ny + self.y, part, self.z_send.at[place, part, way],
            self.z_recv.at[place, part], {"dp": ahead * self.ny + self.y},
        )

    def y_copy(self, place, mine, part):
        side = self.y if mine else self.peer_y
        return self.copy(
            place * self.ny + side, part, self.y_send.at[place, part],
            self.y_recv.at[place, part], {"dp": self.z * self.ny + self.peer_y},
        )

    def x_copy(self, piece, part):
        return self.copy(
            piece, part, self.x_send.at[piece], self.x_recv.at[piece], {"sp": self.across}
        )

    def d_copy(self, piece, part):
        return self.copy(
            piece, part, self.d_send.at[piece, part], self.d_recv.at[piece, part],
            {"sp": self.sibling},
        )

    def greet(self, barrier, ranks):
        sp = (lax.rem(self.rank + 1, ranks), lax.rem(self.rank + ranks - 1, ranks),
              self.sibling, self.across)
        for one in sp:
            pl.semaphore_signal(barrier, inc=1, device_id={"sp": one}, device_id_type=MESH)
        up, down = lax.rem(self.z + 1, self.nz), lax.rem(self.z + self.nz - 1, self.nz)
        for z, y in ((up, self.y), (down, self.y), (self.z, self.peer_y)):
            pl.semaphore_signal(
                barrier, inc=1, device_id={"dp": z * self.ny + y}, device_id_type=MESH
            )
        return 7

    def start(self):
        for part in (0, 1, 2):
            for way in (0, 1):
                @pl.when(self.z < self.nz - 1 if way == 0 else self.z > 0)
                def _():
                    self.z_copy(self.z, part, way).start()

            self.y_copy(self.z, True, part).start()

    def on_z(self, k, part):
        place = self.place(k)
        piece = place * self.ny + self.y
        self.z_copy(place, part, 0).wait_recv()

        @pl.when(jnp.logical_and(place < self.z, self.z < self.nz - 1))
        def _():
            self.z_copy(place, part, 0).start()

        @pl.when(jnp.logical_and(place > self.z, self.z > 0))
        def _():
            self.z_copy(place, part, 1).start()

        self.y_copy(place, True, part).start()
        if part == 0:
            self.x_copy(piece, 0).start()
        self.d_copy(piece, part).start()

    def on_y(self, k, part):
        place = self.place(k)
        piece = place * self.ny + self.peer_y
        self.y_copy(place, False, part).wait_recv()
        if part == 0:
            self.x_copy(piece, 0).start()
        self.d_copy(piece, part).start()

    def piece_at(self, k, mine):
        return self.place(k) * self.ny + (self.y if mine else self.peer_y)

    def on_x(self, k, mine):
        piece = self.piece_at(k, mine)
        self.x_copy(piece, 3).wait_recv()
        self.d_copy(piece, 3).start()

    def landed(self, k, mine):
        piece = self.piece_at(k, mine)
        other = Gather.__new__(Gather)
        other.__dict__.update(self.__dict__)
        other.core = 1 - self.core
        for part in (0, 1, 2, 3):
            other.d_copy(piece, part).wait_recv()

    def finish(self):
        def z_all(k, carry):
            place = self.place(k)
            for part in (0, 1, 2):
                @pl.when(jnp.logical_and(place <= self.z, self.z < self.nz - 1))
                def _():
                    self.z_copy(place, part, 0).wait_send()

                @pl.when(jnp.logical_and(place >= self.z, self.z > 0))
                def _():
                    self.z_copy(place, part, 1).wait_send()

                self.y_copy(place, True, part).wait_send()
            return carry

        lax.fori_loop(0, self.nz, z_all, 0)

        def others(i, carry):
            piece = lax.rem(self.dp + i, self.nz * self.ny)
            self.x_copy(piece, 0).wait_send()
            for part in (0, 1, 2, 3):
                self.d_copy(piece, part).wait_send()
            return carry

        lax.fori_loop(1, self.nz * self.ny, others, 0)


def whole_kernel(ranks, heads, group, nz, ny, *refs):
    (q_hbm, k_hbm, v_hbm, ig_ref, fg_ref, og_hbm, gain_ref, w_hbm), refs = refs[:8], refs[8:]
    out_ref, refs = refs[0], refs[1:]
    (q_ref, k_ref, v_ref, og_ref, w_buf, hid_ref), refs = refs[:6], refs[6:]
    state, refs = refs[:11], refs[11:]
    chain_sems, refs = refs[:4], refs[4:]
    gather_sems, load_sems = refs[:8], refs[8]
    gather = Gather(nz, ny, w_buf, gather_sems)
    barrier = pltpu.get_barrier_semaphore()
    greeted = gather.greet(barrier, ranks)
    w_load = pltpu.make_async_copy(w_hbm, w_buf.at[gather.own], load_sems.at[0])
    loads = [
        pltpu.make_async_copy(src, dst, load_sems.at[1 + i])
        for i, (src, dst) in enumerate(
            ((k_hbm, k_ref), (v_hbm, v_ref), (q_hbm, q_ref), (og_hbm, og_ref))
        )
    ]
    w_load.start()
    for load in loads:
        load.start()
    cell = Cell(
        ranks, heads, group, (q_ref, k_ref, v_ref, ig_ref, fg_ref, og_ref, gain_ref), hid_ref,
        state, chain_sems,
    )
    w_load.wait()
    pl.semaphore_wait(barrier, greeted)
    gather.start()
    cell.gates()
    for load in loads:
        load.wait()
    cell.local_states()

    def project(piece):
        columns = w_buf.shape[2]
        part = pl.ds(pl.multiple_of(piece * columns, columns), columns)
        out_ref[:, part] = nn_dot(hid_ref[...], w_buf[piece]).astype(jnp.bfloat16)

    groups = cell.groups
    mid = groups // 2

    def intra(g):
        return lambda: cell.intra(g)

    def outcome(g):
        return lambda: cell.outcome(g)

    def relays(which, begin, end):
        return lambda: cell.relays(which, begin, end)

    def land(k, mine):
        def work():
            gather.landed(k, mine)
            project(gather.piece_at(k, mine))

        return work

    tasks = []
    for g in range(groups):
        tasks.append([intra(g)])
    tasks[0].append(relays((1,), 0, mid))
    tasks[1].append(relays((1,), mid, groups))
    tasks.append([relays((2,), 0, 1)])
    for g in range(1, groups):
        tasks.append([relays((2,), g, g + 1), relays((3,), g - 1, g), outcome(g - 1)])
    tasks.append([relays((3,), groups - 1, groups), outcome(groups - 1)])
    tasks.append([lambda: project(gather.own)])

    def some(count):
        for _ in range(min(count, len(tasks))):
            for task in tasks.pop(0):
                task()

    for k in range(1, nz):
        for part in (0, 1, 2):
            gather.on_z(k, part)
            gather.on_y(k - 1, part)
            if k > 1 and part == 1:
                gather.on_x(k - 1, True)
                gather.on_x(k - 2, False)
            some(1)
    gather.on_y(nz - 1, 0)
    some(len(tasks))
    gather.on_y(nz - 1, 1)
    gather.on_x(nz - 1, True)
    gather.on_x(nz - 2, False)
    land(1, True)()
    gather.on_y(nz - 1, 2)
    land(0, False)()

    def rest(k, carry):
        land(k, True)()
        land(k - 1, False)()
        return carry

    lax.fori_loop(2, nz, rest, 0)
    gather.on_x(nz - 1, False)
    land(nz - 1, False)()
    cell.finish()
    gather.finish()


def run_whole(ranks, dps, queries, keys, values, in_gate, forget_gate, out_gate, norm_gain, weight):
    seqs, heads, span, size = queries.shape
    items = seqs * heads
    group = 4
    groups = items // group
    ny = 2
    nz = dps // ny
    rows, columns = weight.shape
    vmem = pl.BlockSpec(memory_space=pltpu.VMEM)
    hbm = pl.BlockSpec(memory_space=pl.ANY)
    flat = lambda a: a.reshape((items,) + a.shape[2:])
    dma = pltpu.SemaphoreType.DMA
    big = pltpu.VMEM((items, span, size), jnp.bfloat16)
    return pl.pallas_call(
        functools.partial(whole_kernel, ranks, heads, group, nz, ny),
        out_shape=pltpu.VMEM((seqs * span, dps * columns), jnp.bfloat16),
        in_specs=[hbm, hbm, hbm, vmem, vmem, hbm, vmem, hbm],
        out_specs=vmem,
        scratch_shapes=[
            big, big, big, big,
            pltpu.VMEM((dps, rows, columns), jnp.bfloat16),
            pltpu.VMEM((seqs * span, heads * size), jnp.bfloat16),
            *state_scratch(items, span, size),
            dma((groups,)), dma((groups,)), dma((groups,)), dma((groups,)),
            dma((nz, 3, 2)), dma((nz, 3)), dma((nz, 3)), dma((nz, 3)),
            dma((dps,)), dma((dps,)), dma((dps, 4)), dma((dps, 4)),
            dma((5,)),
        ],
        compiler_params=pltpu.CompilerParams(collective_id=0, has_side_effects=True),
    )(
        flat(queries), flat(keys), flat(values), flat(in_gate), flat(forget_gate),
        flat(out_gate), norm_gain, weight,
    )


def run_cells(ranks, queries, keys, values, in_gate, forget_gate, out_gate, norm_gain):
    seqs, heads, span, head_size = queries.shape
    items = seqs * heads
    group = 4 if heads % 4 == 0 else 1
    groups = items // group
    vmem = pl.BlockSpec(memory_space=pltpu.VMEM)
    flat = lambda a: a.reshape((items,) + a.shape[2:])
    return pl.pallas_call(
        functools.partial(cell_kernel, ranks, heads, group),
        out_shape=jax.ShapeDtypeStruct((seqs * span, heads * head_size), jnp.bfloat16),
        in_specs=[vmem] * 7,
        out_specs=vmem,
        scratch_shapes=[
            *state_scratch(items, span, head_size),
            pltpu.SemaphoreType.DMA((groups,)),
            pltpu.SemaphoreType.DMA((groups,)),
            pltpu.SemaphoreType.DMA((groups,)),
            pltpu.SemaphoreType.DMA((groups,)),
        ],
        compiler_params=pltpu.CompilerParams(collective_id=0, has_side_effects=True),
        cost_estimate=pl.CostEstimate(
            flops=items * span * head_size * 2 * 4 * span, bytes_accessed=40000000, transcendentals=0
        ),
    )(
        flat(queries), flat(keys), flat(values), flat(in_gate), flat(forget_gate),
        flat(out_gate), norm_gain,
    )


def solution(mesh):
    ranks, dps = mesh.shape["sp"], mesh.shape["dp"]

    def body(queries, keys, values, in_gate, forget_gate, out_gate, norm_gain, out_weight):
        seqs, heads, span, head_size = queries.shape
        rows, columns = out_weight.shape
        fits = columns % 128 == 0 and rows % 128 == 0 and dps * rows * columns <= 4 * 2**20
        if ranks == 4 and dps % 2 == 0 and dps >= 6 and heads % 4 == 0 and fits:
            result = run_whole(
                ranks, dps, queries, keys, values, in_gate, forget_gate, out_gate, norm_gain,
                out_weight,
            )
            return result.reshape(seqs, span, -1)
        hidden = run_cells(
            ranks, queries, keys, values, in_gate, forget_gate, out_gate, norm_gain
        )
        result = jnp.dot(
            hidden,
            lax.all_gather(out_weight, "dp", axis=1, tiled=True),
            preferred_element_type=jnp.float32,
        )
        return result.astype(jnp.bfloat16).reshape(seqs, span, -1)

    return jax.shard_map(
        body,
        mesh=mesh,
        in_specs=(
            P("dp", None, "sp", None),
            P("dp", None, "sp", None),
            P("dp", None, "sp", None),
            P("dp", None, "sp"),
            P("dp", None, "sp"),
            P("dp", None, "sp", None),
            P(),
            P(None, "dp"),
        ),
        out_specs=P("dp", "sp", None),
        check_vma=False,
    )
```

```python
import functools

import jax
import jax.numpy as jnp
from jax import lax
from jax.experimental import pallas as pl
from jax.experimental.pallas import tpu as pltpu
from jax.sharding import PartitionSpec as P

norm_eps = 1e-05
MESH = pl.DeviceIdType.MESH
HIGHEST = lax.Precision.HIGHEST
NEG = -1e30


def nt_dot(a, b, precision=None):
    return lax.dot_general(
        a, b, (((1,), (1,)), ((), ())), precision=precision, preferred_element_type=jnp.float32
    )


def tn_dot(a, b):
    return lax.dot_general(a, b, (((0,), (0,)), ((), ())), preferred_element_type=jnp.float32)


def split_dot(dot, wide, narrow):
    high = wide.astype(jnp.bfloat16)
    low = (wide - high.astype(jnp.float32)).astype(jnp.bfloat16)
    return dot(high, narrow) + dot(low, narrow)


def nn_dot(a, b):
    return jnp.dot(a, b, preferred_element_type=jnp.float32)


class Cell:
    def __init__(self, ranks, heads, group, refs, hid_ref, state, sems):
        self.ranks, self.heads, self.group = ranks, heads, group
        self.q, self.k, self.v, self.ig, self.fg, self.og, self.gain = refs
        self.hid = hid_ref
        (self.c_in, self.c_out, self.a_in, self.a_out, self.c_loc, self.n_loc, self.gate_row,
         self.top_row, self.end_row, self.inner, self.stat) = state
        self.sems = sems
        self.rank = lax.axis_index("sp")
        self.items, self.span, self.size = self.q.shape
        self.groups = self.items // group
        self.scale = self.size ** (-0.5)
        self.right = lax.rem(self.rank + 1, ranks)
        self.row_i = lax.broadcasted_iota(jnp.int32, (self.span, self.span), 0)
        self.col_i = lax.broadcasted_iota(jnp.int32, (self.span, self.span), 1)

    def gates(self):
        items, span, size = self.items, self.span, self.size
        logf = jax.nn.log_sigmoid(self.fg[...].astype(jnp.float32))
        cumulative = jnp.dot(
            logf, (self.row_i <= self.col_i).astype(jnp.float32), precision=HIGHEST,
            preferred_element_type=jnp.float32,
        )
        gate = self.ig[...].astype(jnp.float32) - cumulative
        top = jnp.max(gate, axis=1, keepdims=True)
        self.gate_row[...] = gate
        self.top_row[...] = jnp.broadcast_to(top, (items, size))
        self.end_row[...] = jnp.broadcast_to(cumulative[:, span - 1 :], (items, size))
        w_row = jnp.exp(gate - top) * self.scale
        eye = (self.row_i == self.col_i).astype(jnp.float32)
        self.w_col = nt_dot(eye, w_row, precision=HIGHEST)

    def local_states(self):
        for item in range(self.items):
            weighted = self.k[item].astype(jnp.float32) * self.w_col[:, item : item + 1]
            self.n_loc[pl.ds(item, 1), :] = jnp.sum(weighted, axis=0, keepdims=True)
            self.c_loc[item] = split_dot(tn_dot, weighted, self.v[item])

        @pl.when(self.rank == 0)
        def _():
            self.c_in[...] = jnp.zeros_like(self.c_in)
            self.a_in[...] = jnp.zeros_like(self.a_in)

            def first(g, carry):
                self.pass_on(g)
                return carry

            lax.fori_loop(0, self.groups, first, 0)

    def copies(self, g):
        part = pl.ds(g * self.group, self.group)
        c_send, c_recv, a_send, a_recv = self.sems
        return (
            pltpu.make_async_remote_copy(
                src_ref=self.c_out.at[part], dst_ref=self.c_in.at[part],
                send_sem=c_send.at[g], recv_sem=c_recv.at[g],
                device_id={"sp": self.right}, device_id_type=MESH,
            ),
            pltpu.make_async_remote_copy(
                src_ref=self.a_out.at[part], dst_ref=self.a_in.at[part],
                send_sem=a_send.at[g], recv_sem=a_recv.at[g],
                device_id={"sp": self.right}, device_id_type=MESH,
            ),
        )

    def pass_on(self, g):
        for j in range(self.group):
            item = g * self.group + j
            stab = self.a_in[item, 1:2, :]
            top_here = self.top_row[pl.ds(item, 1), :]
            new_top = jnp.maximum(stab, top_here)
            keep = jnp.exp(stab - new_top)
            add = jnp.exp(top_here - new_top)
            self.c_out[item] = (
                keep * self.c_in[item].astype(jnp.float32) + add * self.c_loc[item]
            ).astype(self.c_out.dtype)
            self.a_out[item, 0:1, :] = (
                keep * self.a_in[item, 0:1, :] + add * self.n_loc[pl.ds(item, 1), :]
            )
            self.a_out[item, 1:2, :] = self.end_row[pl.ds(item, 1), :] + new_top
        for copy in self.copies(g):
            copy.start()

    def intra(self, g):
        causal = self.col_i <= self.row_i
        for j in range(self.group):
            item = g * self.group + j
            masked = jnp.where(causal, self.gate_row[pl.ds(item, 1), :], NEG)
            top_p = jnp.max(masked, axis=1, keepdims=True)
            scores = nt_dot(self.q[item], self.k[item]) * (jnp.exp(masked - top_p) * self.scale)
            self.inner[item] = split_dot(nn_dot, scores, self.v[item])
            self.stat[item, :, 0:1] = top_p
            self.stat[item, :, 1:2] = jnp.sum(scores, axis=1, keepdims=True)

    def arrive(self, g):
        for copy in self.copies(g):
            copy.wait_recv()

    def relay(self, g):
        self.arrive(g)
        self.pass_on(g)

    def outcome(self, g):
        for j in range(self.group):
            item = g * self.group + j
            top_p, den = self.stat[item, :, 0:1], self.stat[item, :, 1:2]
            stab = self.a_in[item, 1:2, 0:1]
            both = jnp.maximum(top_p, stab)
            w_intra = jnp.exp(top_p - both)
            w_inter = jnp.exp(stab - both)
            query = self.q[item]
            num = w_inter * nn_dot(query, self.c_in[item]) + w_intra * self.inner[item]
            carried = jnp.sum(
                query.astype(jnp.float32) * self.a_in[item, 0:1, :], axis=1, keepdims=True
            )
            den = w_inter * carried + w_intra * den
            cell = num / jnp.maximum(jnp.abs(den), 1.0)
            cell = cell.astype(jnp.bfloat16).astype(jnp.float32)
            centered = cell - jnp.mean(cell, axis=1, keepdims=True)
            variance = jnp.mean(centered * centered, axis=1, keepdims=True)
            head = lax.rem(item, self.heads)
            seq = item // self.heads
            normed = centered * lax.rsqrt(variance + norm_eps) * self.gain[pl.ds(head, 1), :]
            hidden = normed * jax.nn.sigmoid(self.og[item].astype(jnp.float32))
            self.hid[
                pl.ds(pl.multiple_of(seq * self.span, 16), self.span),
                pl.ds(pl.multiple_of(head * self.size, self.size), self.size),
            ] = hidden.astype(jnp.bfloat16)

    def over(self, work, begin, end):
        def one(g, carry):
            work(g)
            return carry

        lax.fori_loop(begin, end, one, 0)

    def relays(self, ranks, begin, end):
        for rank in ranks:
            @pl.when(self.rank == rank)
            def _():
                self.over(self.relay if rank < self.ranks - 1 else self.arrive, begin, end)

    def finish(self):
        @pl.when(self.rank < self.ranks - 1)
        def _():
            def one(g, carry):
                for copy in self.copies(g):
                    copy.wait_send()
                return carry

            lax.fori_loop(0, self.groups, one, 0)


def state_scratch(items, span, size):
    return [
        pltpu.VMEM((items, size, size), jnp.bfloat16),
        pltpu.VMEM((items, size, size), jnp.bfloat16),
        pltpu.VMEM((items, 8, size), jnp.float32),
        pltpu.VMEM((items, 8, size), jnp.float32),
        pltpu.VMEM((items, size, size), jnp.float32),
        pltpu.VMEM((items, size), jnp.float32),
        pltpu.VMEM((items, span), jnp.float32),
        pltpu.VMEM((items, size), jnp.float32),
        pltpu.VMEM((items, size), jnp.float32),
        pltpu.VMEM((items, span, size), jnp.float32),
        pltpu.VMEM((items, span, size), jnp.float32),
    ]


def cell_kernel(ranks, heads, group, *refs):
    inputs, hid_ref, state, sems = refs[:7], refs[7], refs[8:19], refs[19:23]
    rank = lax.axis_index("sp")
    barrier = pltpu.get_barrier_semaphore()
    for neighbour in (lax.rem(rank + 1, ranks), lax.rem(rank + ranks - 1, ranks)):
        pl.semaphore_signal(barrier, inc=1, device_id={"sp": neighbour}, device_id_type=MESH)
    cell = Cell(ranks, heads, group, inputs, hid_ref, state, sems)
    cell.gates()
    pl.semaphore_wait(barrier, 2)
    cell.local_states()
    cell.over(cell.intra, 0, cell.groups)
    cell.relays(range(1, ranks), 0, cell.groups)
    cell.over(cell.outcome, 0, cell.groups)
    cell.finish()


def nearest(z, nz, k):
    near = jnp.minimum(z, nz - 1 - z)
    half = (k + 1) // 2
    inside = jnp.where(k % 2 == 1, z - half, z + half)
    outside = jnp.where(2 * z < nz, k, nz - 1 - k)
    return jnp.where(k <= 2 * near, inside, outside)


class Gather:
    def __init__(self, nz, ny, w_buf, sems):
        self.nz, self.ny, self.w = nz, ny, w_buf
        (self.z_send, self.z_recv, self.y_send, self.y_recv, self.x_send, self.x_recv,
         self.d_send, self.d_recv) = sems
        self.rank = lax.axis_index("sp")
        self.dp = lax.axis_index("dp")
        self.z, self.y = self.dp // ny, lax.rem(self.dp, ny)
        self.core = lax.rem(self.rank, 2)
        self.plane = lax.rem(self.rank // 2, 2)
        self.sibling = self.rank + 1 - 2 * self.core
        self.across = self.rank + 2 - 4 * self.plane
        self.peer_y = 1 - self.y
        self.rows = w_buf.shape[1] // 2
        self.own = self.dp

    def place(self, k):
        return nearest(self.z, self.nz, k)

    def span_of(self, part):
        quarter = self.rows // 4
        if part == 4:
            return pl.ds(pl.multiple_of((1 - self.core) * self.rows, self.rows), self.rows)
        shift = (3 * self.plane, 1, 2, 3 * (1 - self.plane))[part]
        return pl.ds(pl.multiple_of(self.core * self.rows + shift * quarter, quarter), quarter)

    def area(self, piece, part):
        return self.w.at[piece, self.span_of(part)]

    def copy(self, piece, part, send, recv, where):
        area = self.area(piece, part)
        return pltpu.make_async_remote_copy(
            src_ref=area, dst_ref=area, send_sem=send, recv_sem=recv,
            device_id=where, device_id_type=MESH,
        )

    def z_copy(self, place, part, way):
        ahead = self.z + 1 - 2 * way
        return self.copy(
            place * self.ny + self.y, part, self.z_send.at[place, part, way],
            self.z_recv.at[place, part], {"dp": ahead * self.ny + self.y},
        )

    def y_copy(self, place, mine, part):
        side = self.y if mine else self.peer_y
        return self.copy(
            place * self.ny + side, part, self.y_send.at[place, part],
            self.y_recv.at[place, part], {"dp": self.z * self.ny + self.peer_y},
        )

    def x_copy(self, piece, part):
        return self.copy(
            piece, part, self.x_send.at[piece], self.x_recv.at[piece], {"sp": self.across}
        )

    def d_copy(self, piece, part):
        return self.copy(
            piece, part, self.d_send.at[piece, part], self.d_recv.at[piece, part],
            {"sp": self.sibling},
        )

    def greet(self, barrier, ranks):
        sp = (lax.rem(self.rank + 1, ranks), lax.rem(self.rank + ranks - 1, ranks),
              self.sibling, self.across)
        for one in sp:
            pl.semaphore_signal(barrier, inc=1, device_id={"sp": one}, device_id_type=MESH)
        up, down = lax.rem(self.z + 1, self.nz), lax.rem(self.z + self.nz - 1, self.nz)
        for z, y in ((up, self.y), (down, self.y), (self.z, self.peer_y)):
            pl.semaphore_signal(
                barrier, inc=1, device_id={"dp": z * self.ny + y}, device_id_type=MESH
            )
        return 7

    def start(self, part):
        for way in (0, 1):
            @pl.when(self.z < self.nz - 1 if way == 0 else self.z > 0)
            def _():
                self.z_copy(self.z, part, way).start()

        self.y_copy(self.z, True, part).start()

    def on_z(self, k, part):
        place = self.place(k)
        piece = place * self.ny + self.y
        self.z_copy(place, part, 0).wait_recv()

        @pl.when(jnp.logical_and(place < self.z, self.z < self.nz - 1))
        def _():
            self.z_copy(place, part, 0).start()

        @pl.when(jnp.logical_and(place > self.z, self.z > 0))
        def _():
            self.z_copy(place, part, 1).start()

        self.y_copy(place, True, part).start()
        if part == 0:
            self.x_copy(piece, 0).start()
        self.d_copy(piece, part).start()

    def on_y(self, k, part):
        place = self.place(k)
        piece = place * self.ny + self.peer_y
        self.y_copy(place, False, part).wait_recv()
        if part == 0:
            self.x_copy(piece, 0).start()
        self.d_copy(piece, part).start()

    def piece_at(self, k, mine):
        return self.place(k) * self.ny + (self.y if mine else self.peer_y)

    def on_x(self, k, mine):
        piece = self.piece_at(k, mine)
        self.x_copy(piece, 3).wait_recv()
        self.d_copy(piece, 3).start()

    def landed(self, k, mine):
        piece = self.piece_at(k, mine)
        other = Gather.__new__(Gather)
        other.__dict__.update(self.__dict__)
        other.core = 1 - self.core
        for part in (0, 1, 2, 3):
            other.d_copy(piece, part).wait_recv()

    def finish(self):
        def z_all(k, carry):
            place = self.place(k)
            for part in (0, 1, 2):
                @pl.when(jnp.logical_and(place <= self.z, self.z < self.nz - 1))
                def _():
                    self.z_copy(place, part, 0).wait_send()

                @pl.when(jnp.logical_and(place >= self.z, self.z > 0))
                def _():
                    self.z_copy(place, part, 1).wait_send()

                self.y_copy(place, True, part).wait_send()
            return carry

        lax.fori_loop(0, self.nz, z_all, 0)

        def others(i, carry):
            piece = lax.rem(self.dp + i, self.nz * self.ny)
            self.x_copy(piece, 0).wait_send()
            for part in (0, 1, 2, 3):
                self.d_copy(piece, part).wait_send()
            return carry

        lax.fori_loop(1, self.nz * self.ny, others, 0)


def whole_kernel(ranks, heads, group, nz, ny, *refs):
    (q_hbm, k_hbm, v_hbm, ig_hbm, fg_hbm, og_hbm, gain_hbm, w_hbm), refs = refs[:8], refs[8:]
    out_ref, refs = refs[0], refs[1:]
    (q_ref, k_ref, v_ref, og_ref, ig_ref, fg_ref, gain_ref, w_buf, hid_ref), refs = (
        refs[:9], refs[9:]
    )
    state, refs = refs[:11], refs[11:]
    chain_sems, refs = refs[:4], refs[4:]
    gather_sems, load_sems = refs[:8], refs[8]
    gather = Gather(nz, ny, w_buf, gather_sems)
    barrier = pltpu.get_barrier_semaphore()
    greeted = gather.greet(barrier, ranks)
    w_loads = [
        pltpu.make_async_copy(
            w_hbm.at[gather.span_of(part)], w_buf.at[gather.own, gather.span_of(part)],
            load_sems.at[part],
        )
        for part in range(5)
    ]
    loads = [
        pltpu.make_async_copy(src, dst, load_sems.at[5 + i])
        for i, (src, dst) in enumerate(
            ((fg_hbm, fg_ref), (ig_hbm, ig_ref), (k_hbm, k_ref), (v_hbm, v_ref), (q_hbm, q_ref),
             (gain_hbm, gain_ref), (og_hbm, og_ref))
        )
    ]
    for load in w_loads[:3] + loads + w_loads[3:]:
        load.start()
    cell = Cell(
        ranks, heads, group, (q_ref, k_ref, v_ref, ig_ref, fg_ref, og_ref, gain_ref), hid_ref,
        state, chain_sems,
    )
    pl.semaphore_wait(barrier, greeted)
    for part in (0, 1, 2):
        w_loads[part].wait()
        gather.start(part)
    for load in loads[:2]:
        load.wait()
    cell.gates()
    for load in loads[2:] + w_loads[3:]:
        load.wait()
    cell.local_states()

    def project(piece):
        columns = w_buf.shape[2]
        part = pl.ds(pl.multiple_of(piece * columns, columns), columns)
        out_ref[:, part] = nn_dot(hid_ref[...], w_buf[piece]).astype(jnp.bfloat16)

    groups = cell.groups
    mid = groups // 2

    def intra(g):
        return lambda: cell.intra(g)

    def outcome(g):
        return lambda: cell.outcome(g)

    def relays(which, begin, end):
        return lambda: cell.relays(which, begin, end)

    def land(k, mine):
        def work():
            gather.landed(k, mine)
            project(gather.piece_at(k, mine))

        return work

    tasks = []
    for g in range(groups):
        tasks.append([intra(g)])
    tasks[0].append(relays((1,), 0, mid))
    tasks[1].append(relays((1,), mid, groups))
    tasks.append([relays((2,), 0, 1)])
    for g in range(1, groups):
        tasks.append([relays((2,), g, g + 1), relays((3,), g - 1, g), outcome(g - 1)])
    tasks.append([relays((3,), groups - 1, groups), outcome(groups - 1)])
    tasks.append([lambda: project(gather.own)])

    def some(count):
        for _ in range(min(count, len(tasks))):
            for task in tasks.pop(0):
                task()

    for k in range(1, nz):
        for part in (0, 1, 2):
            gather.on_z(k, part)
            gather.on_y(k - 1, part)
            if k > 1 and part == 1:
                gather.on_x(k - 1, True)
                gather.on_x(k - 2, False)
            some(1)
    gather.on_y(nz - 1, 0)
    some(len(tasks))
    land(1, True)()
    gather.on_y(nz - 1, 1)
    gather.on_x(nz - 1, True)
    gather.on_x(nz - 2, False)
    land(0, False)()

    def rest(k, carry):
        land(k, True)()
        land(k - 1, False)()
        return carry

    lax.fori_loop(2, nz - 1, rest, 0)
    gather.on_y(nz - 1, 2)
    gather.on_x(nz - 1, False)
    rest(nz - 1, 0)
    land(nz - 1, False)()
    cell.finish()
    gather.finish()


def run_whole(ranks, dps, queries, keys, values, in_gate, forget_gate, out_gate, norm_gain, weight):
    seqs, heads, span, size = queries.shape
    items = seqs * heads
    group = 4
    groups = items // group
    ny = 2
    nz = dps // ny
    rows, columns = weight.shape
    vmem = pl.BlockSpec(memory_space=pltpu.VMEM)
    hbm = pl.BlockSpec(memory_space=pl.ANY)
    flat = lambda a: a.reshape((items,) + a.shape[2:])
    dma = pltpu.SemaphoreType.DMA
    big = pltpu.VMEM((items, span, size), jnp.bfloat16)
    return pl.pallas_call(
        functools.partial(whole_kernel, ranks, heads, group, nz, ny),
        out_shape=pltpu.VMEM((seqs * span, dps * columns), jnp.bfloat16),
        in_specs=[hbm] * 8,
        out_specs=vmem,
        scratch_shapes=[
            big, big, big, big,
            pltpu.VMEM((items, span), jnp.bfloat16),
            pltpu.VMEM((items, span), jnp.bfloat16),
            pltpu.VMEM((heads, size), jnp.float32),
            pltpu.VMEM((dps, rows, columns), jnp.bfloat16),
            pltpu.VMEM((seqs * span, heads * size), jnp.bfloat16),
            *state_scratch(items, span, size),
            dma((groups,)), dma((groups,)), dma((groups,)), dma((groups,)),
            dma((nz, 3, 2)), dma((nz, 3)), dma((nz, 3)), dma((nz, 3)),
            dma((dps,)), dma((dps,)), dma((dps, 4)), dma((dps, 4)),
            dma((12,)),
        ],
        compiler_params=pltpu.CompilerParams(collective_id=0, has_side_effects=True),
    )(
        flat(queries), flat(keys), flat(values), flat(in_gate), flat(forget_gate),
        flat(out_gate), norm_gain, weight,
    )


def run_cells(ranks, queries, keys, values, in_gate, forget_gate, out_gate, norm_gain):
    seqs, heads, span, head_size = queries.shape
    items = seqs * heads
    group = 4 if heads % 4 == 0 else 1
    groups = items // group
    vmem = pl.BlockSpec(memory_space=pltpu.VMEM)
    flat = lambda a: a.reshape((items,) + a.shape[2:])
    return pl.pallas_call(
        functools.partial(cell_kernel, ranks, heads, group),
        out_shape=jax.ShapeDtypeStruct((seqs * span, heads * head_size), jnp.bfloat16),
        in_specs=[vmem] * 7,
        out_specs=vmem,
        scratch_shapes=[
            *state_scratch(items, span, head_size),
            pltpu.SemaphoreType.DMA((groups,)),
            pltpu.SemaphoreType.DMA((groups,)),
            pltpu.SemaphoreType.DMA((groups,)),
            pltpu.SemaphoreType.DMA((groups,)),
        ],
        compiler_params=pltpu.CompilerParams(collective_id=0, has_side_effects=True),
        cost_estimate=pl.CostEstimate(
            flops=items * span * head_size * 2 * 4 * span, bytes_accessed=40000000, transcendentals=0
        ),
    )(
        flat(queries), flat(keys), flat(values), flat(in_gate), flat(forget_gate),
        flat(out_gate), norm_gain,
    )


def solution(mesh):
    ranks, dps = mesh.shape["sp"], mesh.shape["dp"]

    def body(queries, keys, values, in_gate, forget_gate, out_gate, norm_gain, out_weight):
        seqs, heads, span, head_size = queries.shape
        rows, columns = out_weight.shape
        fits = columns % 128 == 0 and rows % 128 == 0 and dps * rows * columns <= 4 * 2**20
        if ranks == 4 and dps % 2 == 0 and dps >= 6 and heads % 4 == 0 and fits:
            result = run_whole(
                ranks, dps, queries, keys, values, in_gate, forget_gate, out_gate, norm_gain,
                out_weight,
            )
            return result.reshape(seqs, span, -1)
        hidden = run_cells(
            ranks, queries, keys, values, in_gate, forget_gate, out_gate, norm_gain
        )
        result = jnp.dot(
            hidden,
            lax.all_gather(out_weight, "dp", axis=1, tiled=True),
            preferred_element_type=jnp.float32,
        )
        return result.astype(jnp.bfloat16).reshape(seqs, span, -1)

    return jax.shard_map(
        body,
        mesh=mesh,
        in_specs=(
            P("dp", None, "sp", None),
            P("dp", None, "sp", None),
            P("dp", None, "sp", None),
            P("dp", None, "sp"),
            P("dp", None, "sp"),
            P("dp", None, "sp", None),
            P(),
            P(None, "dp"),
        ),
        out_specs=P("dp", "sp", None),
        check_vma=False,
    )
```
